512 devices in a mesh: sp: 64 (over z, y), tp: 8 (over x, core).
Axes of the slice: x: 4, y: 8, z: 8, core: 2. Of those that a mesh axis runs over, the one named last changes fastest.
Arguments:
- resid: bfloat16 [24576, 2048], P('sp', 'tp'), may hold values from -40 to 40
- query_one: bfloat16 [24576, 1024], P('sp', 'tp'), may hold values from -64 to 64
- key_one: bfloat16 [24576, 1024], P('sp', 'tp'), may hold values from -64 to 64
- query_two: bfloat16 [24576, 1024], P('sp', 'tp'), may hold values from -64 to 64
- key_two: bfloat16 [24576, 1024], P('sp', 'tp'), may hold values from -64 to 64
- values: bfloat16 [24576, 2048], P('sp', 'tp'), may hold values from -6 to 6
- mix_lambda: float32 [8], P('tp'), may hold values from 0.3 to 0.8
- segments: int32 [24576], P('sp'), may hold values from 0 to 31, never falling along the last dimension, each value on 1 to 1536 neighbouring positions
- head_gain: float32 [256], replicated, may hold values from 0.1 to 1.9
- out_weight: bfloat16 [2048, 2048], P(None, 'tp'), may hold values from -0.125 to 0.125
- mixer_gain: float32 [2048], P('tp'), may hold values from 0.1 to 1.9
- gate_weight: bfloat16 [2048, 6144], P('sp', 'tp'), may hold values from -0.125 to 0.125
- up_weight: bfloat16 [2048, 6144], P('sp', 'tp'), may hold values from -0.125 to 0.125
- down_weight: bfloat16 [6144, 2048], P('tp', 'sp'), may hold values from -0.078125 to 0.078125
Outputs:
- layer_out: bfloat16 [24576, 2048], P('sp', 'tp')
The draws below stay inside these ranges and needn't reach their ends.
Inputs may be any that keep to these rules, and one draw needn't show every extreme that they name: `segments`: numbers never fall along the sequence; each document has at most 1536 positions and one has exactly that many.
All inputs are finite; a program needn't handle non-finite values.
Results may differ from the reference program's by a relative error of at most 0.012.
Values may be sent and summed in bfloat16 or wider, within the bound.
A program may use at most 64 MiB of HBM per device.

```python
import math
import jax
import jax.numpy as jnp
import numpy as np
from jax import lax

D = 2048
HEADS = 8
HD = 128
VD = 256
FF = 6144
TOK_DEV = 384
REACH = 4
DOC_MOST = 1536
TOKENS = 24576
DOCS = 32
N_SP = 64
N_TP = 8


def draw_resid(key, part):
    base = jax.random.normal(jax.random.fold_in(key, 11), (TOKENS, D), jnp.float32)
    column = jnp.exp(1.6 * jnp.arange(D, dtype=jnp.float32) / D)
    result = base * column / 2.0
    return jnp.clip(result, -40.0, 40.0).astype(jnp.bfloat16)


def drawn_pair(key, which):
    pair_key = jax.random.fold_in(key, 100 + which)
    width = HEADS * HD
    query = 1.3 * jax.random.normal(jax.random.fold_in(pair_key, 1), (TOKENS, width), jnp.float32)
    keys = 1.3 * jax.random.normal(jax.random.fold_in(pair_key, 2), (TOKENS, width), jnp.float32)
    return (jnp.clip(query, -64.0, 64.0), jnp.clip(keys, -64.0, 64.0))


def draw_query_one(key, part):
    return drawn_pair(key, 1)[0].astype(jnp.bfloat16)


def draw_key_one(key, part):
    return drawn_pair(key, 1)[1].astype(jnp.bfloat16)


def draw_query_two(key, part):
    return drawn_pair(key, 2)[0].astype(jnp.bfloat16)


def draw_key_two(key, part):
    return drawn_pair(key, 2)[1].astype(jnp.bfloat16)


def level_of(own_key, dims, cuts, smallest, largest):
    factor_of = 1.0
    for dim, shards_of in cuts:
        draws = jax.random.uniform(jax.random.fold_in(jax.random.fold_in(own_key, 6), dim), (shards_of,), jnp.float32, smallest / len(cuts), largest / len(cuts))
        factor_of = factor_of * jnp.repeat(jnp.exp(draws), dims[dim] // shards_of).reshape((-1,) + (1,) * (len(dims) - 1 - dim))
    return factor_of


def length_profile(number_of, total, bound, lean):
    weights = [(1 << 20) // math.isqrt(grade ** lean) + 1 for grade in range(2, number_of + 1)]
    rest, counts = total - bound - (number_of - 1), [1] * (number_of - 1)
    while rest > 0:
        movable = [i for i in range(number_of - 1) if counts[i] < bound]
        pool, left = sum([weights[i] for i in movable]), rest
        for i in movable:
            addition = min(bound - counts[i], max(1, left * weights[i] // pool), rest)
            counts[i] = counts[i] + addition
            rest = rest - addition
    return np.array([bound] + counts)


def uneven_parts(rng, count, total, limit, slope):
    if count == 2:
        one = jax.random.randint(rng, (), max(1, total - limit), min(limit, total - 1) + 1)
        return jnp.stack([one, total - one])
    sizes = jnp.asarray(length_profile(count, total, limit, slope), jnp.int32)
    pairs = (count - 1) // 2
    giver, receiver = sizes[1:1 + 2 * pairs:2], sizes[2:2 + 2 * pairs:2]
    slack = jnp.minimum(giver - 1, limit - receiver)
    moved = jax.random.randint(jax.random.fold_in(rng, 1), (pairs,), 0, 1 << 20) % (slack + 1)
    sizes = sizes.at[1:1 + 2 * pairs:2].set(giver - moved).at[2:2 + 2 * pairs:2].set(receiver + moved)
    return sizes[jax.random.permutation(jax.random.fold_in(rng, 2), count)]


def normal_values(stream_key, dims, scale, reach, split=(), kind=jnp.bfloat16):
    values = jax.random.normal(stream_key, dims, jnp.float32) * scale
    if len(split) > 0:
        values = level_of(stream_key, dims, split, -0.22, 0.18) * values
    return jnp.clip(values, min=-reach, max=reach).astype(kind)


def setup_inputs(seed: int = 0) -> dict:
    arg_keys = jax.random.split(jax.random.key(seed), 15)
    resid = draw_resid(jax.random.fold_in(arg_keys[14], 71), 0)
    query_one = draw_query_one(jax.random.fold_in(arg_keys[14], 71), 0)
    key_one = draw_key_one(jax.random.fold_in(arg_keys[14], 71), 0)
    query_two = draw_query_two(jax.random.fold_in(arg_keys[14], 71), 0)
    key_two = draw_key_two(jax.random.fold_in(arg_keys[14], 71), 0)
    values = normal_values(arg_keys[5], (TOKENS, HEADS * VD), 1.0, 6.0, ((0, 64), (1, 8)))
    mix_lambda = jnp.clip(0.3 + 0.5 * jax.random.uniform(arg_keys[6], (HEADS,), jnp.float32) ** level_of(arg_keys[6], (HEADS,), ((0, 8),), -0.2, 0.2), 0.3, 0.8)
    segments = jnp.searchsorted(jnp.cumsum(uneven_parts(arg_keys[7], DOCS, TOKENS, DOC_MOST, 0)), jnp.arange(TOKENS), side="right").astype(jnp.int32)
    head_gain = jnp.clip(1.0 + 0.18 * jax.random.normal(arg_keys[8], (VD,), jnp.float32), 0.1, 1.9)
    out_weight = normal_values(arg_keys[9], (HEADS * VD, D), (HEADS * VD) ** -0.5, 0.125, ((1, 8),))
    mixer_gain = jnp.clip(1.0 + 0.18 * jax.random.normal(arg_keys[10], (D,), jnp.float32), 0.1, 1.9)
    gate_weight = normal_values(arg_keys[11], (D, FF), D ** -0.5, 0.125, ((0, 64), (1, 8)))
    up_weight = normal_values(arg_keys[12], (D, FF), D ** -0.5, 0.125, ((0, 64), (1, 8)))
    down_weight = normal_values(arg_keys[13], (FF, D), FF ** -0.5, 0.078125, ((0, 8), (1, 64)))
    return {"resid": resid, "query_one": query_one, "key_one": key_one, "query_two": query_two, "key_two": key_two, "values": values, "mix_lambda": mix_lambda, "segments": segments, "head_gain": head_gain, "out_weight": out_weight, "mixer_gain": mixer_gain, "gate_weight": gate_weight, "up_weight": up_weight, "down_weight": down_weight}


def reference(resid, query_one, key_one, query_two, key_two, values, mix_lambda, segments, head_gain, out_weight, mixer_gain, gate_weight, up_weight, down_weight):
    rows = TOK_DEV
    span = REACH * TOK_DEV

    def padded(array):
        return jnp.concatenate([jnp.zeros((span,) + array.shape[1:], array.dtype), array], 0)
    key_first = padded(key_one)
    key_second = padded(key_two)
    value_pad = padded(values)
    seg_pad = jnp.concatenate([jnp.full((span,), -1, jnp.int32), segments.astype(jnp.int32)], 0)

    def block(index):
        start = (index * rows).astype(jnp.int32)
        width = span + rows
        q_first = lax.dynamic_slice_in_dim(query_one, start, rows, 0).reshape(rows, HEADS, HD).astype(jnp.float32)
        q_second = lax.dynamic_slice_in_dim(query_two, start, rows, 0).reshape(rows, HEADS, HD).astype(jnp.float32)
        k_first = lax.dynamic_slice_in_dim(key_first, start, width, 0).reshape(width, HEADS, HD).astype(jnp.float32)
        k_second = lax.dynamic_slice_in_dim(key_second, start, width, 0).reshape(width, HEADS, HD).astype(jnp.float32)
        vals = lax.dynamic_slice_in_dim(value_pad, start, width, 0).reshape(width, HEADS, VD).astype(jnp.float32)
        seg_query = lax.dynamic_slice_in_dim(segments.astype(jnp.int32), start, rows, 0)
        seg_key = lax.dynamic_slice_in_dim(seg_pad, start, width, 0)
        q_pos = start + jnp.arange(rows, dtype=jnp.int32)
        k_pos = start - span + jnp.arange(width, dtype=jnp.int32)
        allowed = (seg_key[None, :] == seg_query[:, None]) & (k_pos[None, :] <= q_pos[:, None]) & (k_pos[None, :] >= 0)

        def weights(query, keys):
            score = jnp.einsum('qhd,khd->hqk', query, keys) * HD ** (-0.5)
            score = jnp.where(allowed[None], score, -jnp.inf)
            score = score - lax.optimization_barrier(jnp.max(score, axis=-1, keepdims=True))
            expo = jnp.exp(score)
            return (expo / lax.optimization_barrier(jnp.sum(expo, axis=-1, keepdims=True))).astype(jnp.bfloat16)
        probs_first = weights(q_first, k_first).astype(jnp.float32)
        probs_second = weights(q_second, k_second).astype(jnp.float32)
        out_first = jnp.einsum('hqk,khe->qhe', probs_first, vals)
        out_second = jnp.einsum('hqk,khe->qhe', probs_second, vals)
        head_out = out_first - mix_lambda[None, :, None] * out_second
        meansq = lax.optimization_barrier(jnp.mean(head_out * head_out, axis=-1, keepdims=True))
        normal = head_out * lax.rsqrt(meansq + 1e-05) * head_gain
        return normal.reshape(rows, HEADS * VD).astype(jnp.bfloat16)
    attn_rows = lax.map(block, jnp.arange(N_SP, dtype=jnp.int32)).reshape(TOKENS, HEADS * VD)
    mid = (resid.astype(jnp.float32) + jnp.dot(attn_rows, out_weight, preferred_element_type=jnp.float32)).astype(jnp.bfloat16)
    midf = mid.astype(jnp.float32)
    meansq = lax.optimization_barrier(jnp.mean(midf * midf, axis=-1, keepdims=True))
    normed = (midf * lax.rsqrt(meansq + 1e-06) * mixer_gain).astype(jnp.bfloat16)
    gate = jnp.dot(normed, gate_weight, preferred_element_type=jnp.float32)
    up = jnp.dot(normed, up_weight, preferred_element_type=jnp.float32)
    hidden = (jax.nn.silu(gate) * up).astype(jnp.bfloat16)
    blocks = FF // N_TP
    hidden_blocks = hidden.reshape(TOKENS, N_TP, blocks).transpose(1, 0, 2)
    down_blocks = down_weight.reshape(N_TP, blocks, D)

    def add_block(total, pair):
        part = jnp.dot(pair[0], pair[1], preferred_element_type=jnp.float32).astype(jnp.bfloat16)
        part = lax.optimization_barrier(part)
        return (total + part.astype(jnp.float32), None)
    summed, unused = lax.scan(add_block, jnp.zeros((TOKENS, D), jnp.float32), (hidden_blocks, down_blocks))
    return (midf + summed).astype(jnp.bfloat16)
```

```python
import functools

import jax
import jax.numpy as jnp
from jax import lax
from jax.experimental import pallas as pl
from jax.experimental.pallas import tpu as pltpu
from jax.sharding import PartitionSpec as P

MESH = pl.DeviceIdType.MESH
BF, F32 = jnp.bfloat16, jnp.float32
ROWS, HALF, HD, VD = 384, 192, 128, 256
REACH = 4
BW, AW, GU = 1280, 1024, 768
YM, YP, ZM, ZP = 5, 2, 4, 3
NT = (((1,), (1,)), ((), ()))


def dot(a, b):
    return jnp.dot(a, b, preferred_element_type=F32)


def dot_nt(a, b):
    return lax.dot_general(a, b, NT, preferred_element_type=F32)


def kernel(
    q1_h, q2_h, k1_h, k2_h, v_h, resid_h, wout_h, gate_h, up_h, down_h, seg_h, hg, mg, lam,
    out_ref,
    q1, q2, resid, wout, dwn, kbuf, vbuf, gbuf, bbuf, abuf, segq, gains, mref, lref, oacc,
    heads, mids, xn, hid, pown, psend, precv, stage, rhalf, rfull,
    loc, kv_s, kv_r, b1m_s, b1m_r, b1p_s, b1p_r, a1m_s, a1m_r, a1p_s, a1p_r,
    b20_s, b20_r, a20_s, a20_r, b2m_s, b2m_r, b2p_s, b2p_r, a2m_s, a2m_r, a2p_s, a2p_r,
    xg_s, xg_r, d_s, d_r, rs_s, rs_r,
):
    s, t = lax.axis_index("sp"), lax.axis_index("tp")
    z, y = lax.div(s, 8), lax.rem(s, 8)
    x, c = lax.div(t, 2), lax.rem(t, 2)
    o = 1 - c

    def ring(i, by, n):
        return lax.rem(i + (by % n), n)

    yp, ym = {"sp": z * 8 + ring(y, 1, 8)}, {"sp": z * 8 + ring(y, -1, 8)}
    zp, zm = {"sp": ring(z, 1, 8) * 8 + y}, {"sp": ring(z, -1, 8) * 8 + y}
    kp, km = {"sp": ring(s, 1, 64)}, {"sp": ring(s, -1, 64)}
    xp, xm = {"tp": ring(x, 1, 4) * 2 + c}, {"tp": ring(x, -1, 4) * 2 + c}
    pc = {"tp": x * 2 + o}

    barrier = pltpu.get_barrier_semaphore()
    for dev in (yp, ym, zp, zm, kp, km, xp, xm, pc):
        pl.semaphore_signal(barrier, inc=1, device_id=dev, device_id_type=MESH)

    loads = [
        (k1_h, kbuf.at[0, :, 0:HD]),
        (k2_h, kbuf.at[0, :, HD : 2 * HD]),
        (v_h, vbuf.at[0]),
        (gate_h, bbuf.at[z, y, :, 0:GU]),
        (up_h, abuf.at[z, y, :, 0:GU]),
        (seg_h, gbuf.at[0]),
        (down_h, dwn),
        (q1_h, q1),
        (q2_h, q2),
        (resid_h, resid),
        (wout_h, wout),
    ]
    loads = [pltpu.make_async_copy(a, b, loc.at[i]) for i, (a, b) in enumerate(loads)]
    for i in (6, 3, 4, 0, 1, 2, 5, 7, 8, 9, 10):
        loads[i].start()

    gains[t] = jnp.broadcast_to(mg[...], (16, VD))
    loads[6].wait()
    eye = (
        lax.broadcasted_iota(jnp.int32, (32, 32), 0) == lax.broadcasted_iota(jnp.int32, (32, 32), 1)
    )
    turned = dot_nt(jnp.where(eye, 1.0, 0.0).astype(BF), dwn[...]).astype(BF)
    bbuf[z, y, :, GU:BW] = turned[:, : BW - GU]
    abuf[z, y, :, GU:AW] = turned[:, BW - GU :]
    for i in (3, 4, 0, 1, 2, 5):
        loads[i].wait()
    pl.semaphore_wait(barrier, 9)

    pending = []

    def copy(src, dst, ss, rs, dev):
        return pltpu.make_async_remote_copy(
            src_ref=src, dst_ref=dst, send_sem=ss, recv_sem=rs, device_id=dev, device_id_type=MESH
        )

    def send(src, dst, ss, rs, dev):
        one = copy(src, dst, ss, rs, dev)
        one.start()
        pending.append(one)

    def got(ref, ss, rs):
        copy(ref, ref, ss, rs, pc).wait_recv()

    def b_first(which, hop):
        dev, ss, rs, last, step = (
            (ym, b1m_s, b1m_r, YM, 1) if which else (yp, b1p_s, b1p_r, YP, -1)
        )
        shard = y if hop < 0 else ring(y, step * (hop + 1), 8)
        ref = bbuf.at[z, shard]
        if hop >= 0:
            got(ref, ss.at[hop], rs.at[hop])
        if hop + 1 < last:
            send(ref, ref, ss.at[hop + 1], rs.at[hop + 1], dev)
        if hop >= 0 or which:
            for k, far in enumerate((zm, zp)):
                copy(ref, ref, b20_s.at[k], b20_r.at[k], far).start()

    def a_first(which, hop):
        dev, ss, rs, last, step = (
            (zm, a1m_s, a1m_r, ZM, 1) if which else (zp, a1p_s, a1p_r, ZP, -1)
        )
        shard = z if hop < 0 else ring(z, step * (hop + 1), 8)
        ref = abuf.at[shard, y]
        if hop >= 0:
            got(ref, ss.at[hop], rs.at[hop])
        if hop + 1 < last:
            send(ref, ref, ss.at[hop + 1], rs.at[hop + 1], dev)
        if hop >= 0 or which:
            copy(ref, ref, a20_s, a20_r, ym).start()

    def b_part(row, k):
        return bbuf.at[row, :, :, 0:GU] if k == 0 else bbuf.at[row, :, :, GU:BW]

    def a_part(col, k):
        return abuf.at[:, col, :, 0:GU] if k == 0 else abuf.at[:, col, :, GU:AW]

    def b_second(which, hop, part):
        dev, ss, rs, last, step = (
            (zm, b2m_s, b2m_r, ZM, 1) if which else (zp, b2p_s, b2p_r, ZP, -1)
        )
        row = ring(z, step * (hop + 1), 8)
        if hop == 0:
            k = 0 if which else 1
            got(bbuf.at[row], b20_s.at[k], b20_r.at[k])
        else:
            got(b_part(row, part), ss.at[hop, part], rs.at[hop, part])
        for k in (0, 1) if hop == 0 else (part,):
            if hop + 1 < last:
                ref = b_part(row, k)
                send(ref, ref, ss.at[hop + 1, k], rs.at[hop + 1, k], dev)

    def a_second(which, hop, part):
        dev, ss, rs, last, step = (
            (ym, a2m_s, a2m_r, YM, 1) if which else (yp, a2p_s, a2p_r, YP, -1)
        )
        col = ring(y, step * (hop + 1), 8)
        if hop == 0 and which:
            got(abuf.at[:, col], a20_s, a20_r)
        else:
            got(a_part(col, part), ss.at[hop, part], rs.at[hop, part])
        for k in (0, 1) if hop == 0 and which else (part,):
            if hop + 1 < last:
                ref = a_part(col, k)
                send(ref, ref, ss.at[hop + 1, k], rs.at[hop + 1, k], dev)

    def a_own():
        for k in (0, 1):
            ref = a_part(y, k)
            send(ref, ref, a2p_s.at[0, k], a2p_r.at[0, k], yp)

    def kv(slot, part):
        bufs = ((0, kbuf), (2, gbuf)) if part == 0 else ((1, vbuf),)
        for i, buf in bufs:
            if slot > 0:
                got(buf.at[slot], kv_s.at[i, slot], kv_r.at[i, slot])
            if slot < REACH:
                send(buf.at[slot], buf.at[slot + 1], kv_s.at[i, slot + 1], kv_r.at[i, slot + 1], kp)

    def attend(k):
        ids = gbuf[k].astype(F32) + jnp.where(s >= k, 0.0, 1000.0)

        def chunk(i, carry):
            rows = pl.ds(pl.multiple_of(i * 128, 128), 128)
            same = segq[rows, 0:1] == ids
            if k == 0:
                qpos = i * 128 + lax.broadcasted_iota(jnp.int32, (128, ROWS), 0)
                same = same & (lax.broadcasted_iota(jnp.int32, (128, ROWS), 1) <= qpos)
            for m, q in enumerate((q1, q2)):
                score = dot_nt(q[rows, :], kbuf[k, :, m * HD : (m + 1) * HD])
                score = jnp.where(same, score * (HD**-0.5 * 1.4426950408889634), -jnp.inf)
                top = jnp.max(score, axis=1, keepdims=True)
                if k > 0:
                    before = mref[m, rows, 0:1]
                    top = jnp.maximum(top, before)
                expo = jnp.exp2(score - top)
                total = jnp.sum(expo, axis=1, keepdims=True)
                value = dot(expo.astype(BF), vbuf[k])
                if k > 0:
                    scale = jnp.exp2(before - top)
                    total = total + scale * lref[m, rows, 0:1]
                    value = value + scale * oacc[m, rows, :]
                mref[m, rows, :] = jnp.broadcast_to(top, (128, 128))
                lref[m, rows, :] = jnp.broadcast_to(total, (128, 128))
                oacc[m, rows, :] = value
            return carry

        lax.fori_loop(0, 3, chunk, 0)

    def finish_heads():
        def chunk(i, carry):
            rows = pl.ds(pl.multiple_of(i * 64, 64), 64)
            head = oacc[0, rows, :] / lref[0, rows, 0:1]
            head = head - lam[0] * (oacc[1, rows, :] / lref[1, rows, 0:1])
            meansq = jnp.mean(head * head, axis=1, keepdims=True)
            heads[t, rows, :] = (head * lax.rsqrt(meansq + 1e-05) * hg[...]).astype(BF)
            return carry

        lax.fori_loop(0, 6, chunk, 0)

    def slot_of(by, core):
        return ring(x, by, 4) * 2 + core

    def x_gather(buf, g):
        n = buf.shape[1]
        low, high = pl.ds(0, n // 2), pl.ds(n // 2, n // 2)

        def go(ref, i, dev):
            send(ref, ref, xg_s.at[g, i], xg_r.at[g, i], dev)

        def come(ref, i):
            got(ref, xg_s.at[g, i], xg_r.at[g, i])

        def own():
            go(buf.at[t], 0, xp)
            go(buf.at[t], 1, xm)
            go(buf.at[t], 4, pc)

        def near():
            a, b = buf.at[slot_of(-1, c)], buf.at[slot_of(1, c)]
            come(a, 0)
            go(buf.at[slot_of(-1, c), low], 2, xp)
            go(a, 5, pc)
            come(b, 1)
            go(buf.at[slot_of(1, c), high], 3, xm)
            go(b, 6, pc)

        def far():
            for i, part in ((2, low), (3, high)):
                ref = buf.at[slot_of(2, c), part]
                come(ref, i)
                go(ref, i + 5, pc)

        def across():
            come(buf.at[slot_of(0, o)], 4)
            come(buf.at[slot_of(-1, o)], 5)
            come(buf.at[slot_of(1, o)], 6)

        def across_far():
            for i, part in ((2, low), (3, high)):
                come(buf.at[slot_of(2, o), part], i + 5)

        return own, near, far, across, across_far

    gain_g = x_gather(gains, 0)
    head_g = x_gather(heads, 1)
    mid_g = x_gather(mids, 2)

    def project(slots, first):
        total = None if first else oacc[0]
        for by, core in slots:
            i = slot_of(by, core)
            w = wout[pl.ds(pl.multiple_of(i * VD, VD), VD), :]
            part = dot(heads[i], w)
            total = part if total is None else total + part
        oacc[0] = total

    def project_near():
        project(((0, c), (-1, c), (1, c), (0, o), (-1, o), (1, o)), True)

    def project_far():
        project(((2, c), (2, o)), False)
        mids[t] = (resid[...].astype(F32) + oacc[0]).astype(BF)

    def normalise():
        def chunk(i, carry):
            rows = pl.ds(pl.multiple_of(i * 32, 32), 32)
            mid = [mids[j, rows, :].astype(F32) for j in range(8)]
            squares = sum([m * m for m in mid])
            meansq = jnp.sum(squares, axis=1, keepdims=True) * (1.0 / (8 * VD))
            scale = lax.rsqrt(meansq + 1e-06)
            for j in range(8):
                gain = gains[j][0:1, :]
                xn[rows, j * VD : (j + 1) * VD] = (mid[j] * scale * gain).astype(BF)
            return carry

        lax.fori_loop(0, 12, chunk, 0)

    def hidden():
        def tile(i, carry):
            cols = pl.ds(pl.multiple_of(i * 256, 256), 256)
            gate = dot(xn[...], bbuf[:, :, :, cols].reshape(2048, 256))
            up = dot(xn[...], abuf[:, :, :, cols].reshape(2048, 256))
            hid[:, cols] = (gate / (1.0 + jnp.exp(-gate)) * up).astype(BF)
            return carry

        lax.fori_loop(0, 3, tile, 0)

    def terms(i):
        one = dot_nt(hid[:, 0 : BW - GU], bbuf[i, :, :, GU:BW].reshape(256, BW - GU))
        return one + dot_nt(hid[:, BW - GU :], abuf[i, :, :, GU:AW].reshape(256, AW - GU))

    events = []

    def at(time, what, *args):
        events.append((time, len(events), what, args))

    for hop in range(YM):
        at(3.5 * (hop + 1), b_first, True, hop)
        if hop < YP:
            at(3.5 * (hop + 1) + 0.1, b_first, False, hop)
        if hop < ZM:
            at(3.5 * (hop + 1) + 0.2, a_first, True, hop)
        if hop < ZP:
            at(3.5 * (hop + 1) + 0.3, a_first, False, hop)
    at(2.0, gain_g[0])
    at(7.5, gain_g[1])
    at(11.0, gain_g[2])
    at(11.1, gain_g[3])
    at(14.5, gain_g[4])
    at(2.1, attend, 0)
    for slot, (tk, tv) in enumerate(((7.7, 12.0), (18.0, 22.0), (26.3, 30.5), (34.7, 39.0))):
        at(tk, kv, slot + 1, 0)
        at(tv, kv, slot + 1, 1)
        at(tv + 0.1, attend, slot + 1)
    at(30.6, a_own)
    for which, times in ((True, ((22, 22), (32.5, 38), (46.5, 52.5), (60.5, 66))),
                         (False, ((22.1, 22.1), (32.6, 38.1), (46.6, 52.6)))):
        for hop, pair in enumerate(times):
            at(pair[0], b_second, which, hop, 0)
            if hop:
                at(pair[1], b_second, which, hop, 1)
    for which, times in ((True, ((20, 20), (30.7, 33.7), (42, 45), (53, 56), (60.4, 67))),
                         (False, ((48, 51), (60.3, 65)))):
        for hop, pair in enumerate(times):
            at(pair[0], a_second, which, hop, 0)
            if hop or not which:
                at(pair[1], a_second, which, hop, 1)
    at(40.0, finish_heads)
    at(40.1, head_g[0])
    at(46.0, head_g[1])
    at(47.0, head_g[3])
    at(47.1, project_near)
    at(48.5, head_g[2])
    at(49.5, head_g[4])
    at(49.6, project_far)
    at(49.7, mid_g[0])
    at(55.5, mid_g[1])
    at(58.0, mid_g[2])
    at(59.0, mid_g[3])
    at(59.1, mid_g[4])
    at(59.2, normalise)
    at(61.0, hidden)

    b_first(True, -1)
    b_first(False, -1)
    a_first(True, -1)
    a_first(False, -1)
    kv(0, 0)
    kv(0, 1)
    for i in (7, 8):
        loads[i].wait()
    ids = jnp.broadcast_to(gbuf[0].astype(F32), (128, ROWS))
    segq[...] = ids.T
    for i in (9, 10):
        loads[i].wait()
    for _, _, what, args in sorted(events, key=lambda e: e[:2]):
        what(*args)

    chips = (2, 1, -1, 0)
    for i, by in enumerate(chips):
        psend[i] = terms(slot_of(by, o)).astype(BF)
        send(psend.at[i], precv.at[i], d_s.at[i], d_r.at[i], pc)
        pown[i] = terms(slot_of(by, c))
    low, high = pl.ds(0, HALF), pl.ds(HALF, HALF)

    def pair(i, part):
        return pown[i, part, :] + precv[i, part, :].astype(F32)

    got(precv.at[0], d_s.at[0], d_r.at[0])
    stage[0, low, :] = pair(0, low).astype(BF)
    send(stage.at[0, low], rhalf.at[0], rs_s.at[0], rs_r.at[0], xp)
    stage[0, high, :] = pair(0, high).astype(BF)
    send(stage.at[0, high], rhalf.at[1], rs_s.at[1], rs_r.at[1], xm)
    got(precv.at[1], d_s.at[1], d_r.at[1])
    stage[1, high, :] = pair(1, high).astype(BF)
    send(stage.at[1, high], rfull.at[0, high], rs_s.at[2], rs_r.at[2], xp)
    got(precv.at[2], d_s.at[2], d_r.at[2])
    stage[2, low, :] = pair(2, low).astype(BF)
    send(stage.at[2, low], rfull.at[1, low], rs_s.at[3], rs_r.at[3], xm)
    got(rhalf.at[0], rs_s.at[0], rs_r.at[0])
    stage[1, low, :] = (pair(1, low) + rhalf[0].astype(F32)).astype(BF)
    send(stage.at[1, low], rfull.at[0, low], rs_s.at[4], rs_r.at[4], xp)
    got(rhalf.at[1], rs_s.at[1], rs_r.at[1])
    stage[2, high, :] = (pair(2, high) + rhalf[1].astype(F32)).astype(BF)
    send(stage.at[2, high], rfull.at[1, high], rs_s.at[5], rs_r.at[5], xm)
    got(precv.at[3], d_s.at[3], d_r.at[3])
    pown[3] = pown[3] + precv[3].astype(F32) + mids[t].astype(F32)
    got(rfull.at[0, high], rs_s.at[2], rs_r.at[2])
    got(rfull.at[1, low], rs_s.at[3], rs_r.at[3])
    got(rfull.at[0, low], rs_s.at[4], rs_r.at[4])
    got(rfull.at[1, high], rs_s.at[5], rs_r.at[5])
    out_ref[...] = (pown[3] + rfull[0].astype(F32) + rfull[1].astype(F32)).astype(BF)

    for one in pending:
        one.wait_send()
    copy(bbuf.at[z], bbuf.at[z], b20_s.at[0], b20_r.at[0], zm).wait_send()
    copy(bbuf.at[z], bbuf.at[z], b20_s.at[1], b20_r.at[1], zp).wait_send()
    copy(abuf.at[:, y], abuf.at[:, y], a20_s, a20_r, ym).wait_send()


def body(
    resid, query_one, key_one, query_two, key_two, values, mix_lambda, segments, head_gain,
    out_weight, mixer_gain, gate_weight, up_weight, down_weight,
):
    hbm = pl.BlockSpec(memory_space=pltpu.HBM)
    vmem = pl.BlockSpec(memory_space=pltpu.VMEM)
    dma = pltpu.SemaphoreType.DMA
    scratch = [
        pltpu.VMEM((ROWS, HD), BF), pltpu.VMEM((ROWS, HD), BF), pltpu.VMEM((ROWS, VD), BF),
        pltpu.VMEM((2048, VD), BF), pltpu.VMEM((768, 32), BF),
        pltpu.VMEM((5, ROWS, 2 * HD), BF), pltpu.VMEM((5, ROWS, VD), BF),
        pltpu.VMEM((5, 1, ROWS), jnp.int32),
        pltpu.VMEM((8, 8, 32, BW), BF), pltpu.VMEM((8, 8, 32, AW), BF),
        pltpu.VMEM((ROWS, 128), F32), pltpu.VMEM((8, 16, VD), F32),
        pltpu.VMEM((2, ROWS, 128), F32), pltpu.VMEM((2, ROWS, 128), F32),
        pltpu.VMEM((2, ROWS, VD), F32),
        pltpu.VMEM((8, ROWS, VD), BF), pltpu.VMEM((8, ROWS, VD), BF),
        pltpu.VMEM((ROWS, 2048), BF), pltpu.VMEM((ROWS, 768), BF),
        pltpu.VMEM((4, ROWS, VD), F32), pltpu.VMEM((4, ROWS, VD), BF),
        pltpu.VMEM((4, ROWS, VD), BF), pltpu.VMEM((3, ROWS, VD), BF),
        pltpu.VMEM((2, HALF, VD), BF), pltpu.VMEM((2, ROWS, VD), BF),
        dma((11,)), dma((3, 5)), dma((3, 5)),
        dma((YM,)), dma((YM,)), dma((YP,)), dma((YP,)),
        dma((ZM,)), dma((ZM,)), dma((ZP,)), dma((ZP,)),
        dma((2,)), dma((2,)), dma, dma,
        dma((ZM, 2)), dma((ZM, 2)), dma((ZP, 2)), dma((ZP, 2)),
        dma((YM, 2)), dma((YM, 2)), dma((YP, 2)), dma((YP, 2)),
        dma((3, 9)), dma((3, 9)), dma((4,)), dma((4,)), dma((6,)), dma((6,)),
    ]
    return pl.pallas_call(
        kernel,
        name="layer",
        out_shape=jax.ShapeDtypeStruct((ROWS, VD), BF),
        in_specs=[hbm] * 11 + [vmem] * 2 + [pl.BlockSpec(memory_space=pltpu.SMEM)],
        out_specs=vmem,
        scratch_shapes=scratch,
        compiler_params=pltpu.CompilerParams(collective_id=0, has_side_effects=True),
    )(
        query_one, query_two, key_one, key_two, values, resid, out_weight, gate_weight,
        up_weight, down_weight, segments.reshape(1, -1), head_gain.reshape(1, -1),
        mixer_gain.reshape(1, -1), mix_lambda,
    )


def solution(mesh):
    in_specs = (
        P("sp", "tp"), P("sp", "tp"), P("sp", "tp"), P("sp", "tp"), P("sp", "tp"), P("sp", "tp"),
        P("tp"), P("sp"), P(), P(None, "tp"), P("tp"), P("sp", "tp"), P("sp", "tp"), P("tp", "sp"),
    )
    return jax.shard_map(
        body, mesh=mesh, in_specs=in_specs, out_specs=P("sp", "tp"), check_vma=False
    )
```

```python
import functools

import jax
import jax.numpy as jnp
from jax import lax
from jax.experimental import pallas as pl
from jax.experimental.pallas import tpu as pltpu
from jax.sharding import PartitionSpec as P

MESH = pl.DeviceIdType.MESH
BF, F32 = jnp.bfloat16, jnp.float32
ROWS, HD, VD = 384, 128, 256
REACH = 4
BW, AW, GU = 1152, 1152, 768
YM, YP, ZM, ZP = 5, 2, 5, 2
CH, QU = 192, 96
NT = (((1,), (1,)), ((), ()))


def dot(a, b):
    return jnp.dot(a, b, preferred_element_type=F32)


def dot_nt(a, b):
    return lax.dot_general(a, b, NT, preferred_element_type=F32)


def kernel(
    q1_h, q2_h, k1_h, k2_h, v_h, resid_h, wout_h, gate_h, up_h, down_h, seg_h, hg, mg, lam,
    out_ref,
    q1, q2, resid, wout, kbuf, vbuf, gbuf, bbuf, abuf, segq, gains, mref, lref, oacc,
    heads, mids, xn, hid, pown, psend, precv, stage, rhalf, rfull,
    loc, kv_s, kv_r, b1m_s, b1m_r, b1p_s, b1p_r, a1m_s, a1m_r, a1p_s, a1p_r,
    b20_s, b20_r, a20_s, a20_r, b2m_s, b2m_r, b2p_s, b2p_r, a2m_s, a2m_r, a2p_s, a2p_r,
    xg_s, xg_r, d_s, d_r, rs_s, rs_r,
):
    s, t = lax.axis_index("sp"), lax.axis_index("tp")
    z, y = lax.div(s, 8), lax.rem(s, 8)
    x, c = lax.div(t, 2), lax.rem(t, 2)
    o = 1 - c

    def ring(i, by, n):
        return lax.rem(i + (by % n), n)

    yp, ym = {"sp": z * 8 + ring(y, 1, 8)}, {"sp": z * 8 + ring(y, -1, 8)}
    zp, zm = {"sp": ring(z, 1, 8) * 8 + y}, {"sp": ring(z, -1, 8) * 8 + y}
    last, wrap = y == 7, jnp.where(y == 7, REACH, 0)
    turn = {"sp": jnp.where(last, ring(z, 1, 8) * 8 + y, z * 8 + ring(y, 1, 8))}
    xp, xm = {"tp": ring(x, 1, 4) * 2 + c}, {"tp": ring(x, -1, 4) * 2 + c}
    pc = {"tp": x * 2 + o}

    barrier = pltpu.get_barrier_semaphore()
    for dev in (yp, ym, zp, zm, xp, xm, pc):
        pl.semaphore_signal(barrier, inc=1, device_id=dev, device_id_type=MESH)

    loads = [
        (k1_h, kbuf.at[0, :, 0:HD]),
        (k2_h, kbuf.at[0, :, HD : 2 * HD]),
        (v_h, vbuf.at[0]),
        (gate_h, bbuf.at[z, y, :, 0:GU]),
        (up_h, abuf.at[z, y, :, 0:GU]),
        (seg_h, gbuf.at[0, 0]),
        (down_h.at[:, 0 : BW - GU], bbuf.at[z, y, :, GU:BW]),
        (down_h.at[:, BW - GU :], abuf.at[z, y, :, GU:AW]),
        (q1_h, q1),
        (q2_h, q2),
        (resid_h, resid),
        (wout_h, wout),
    ]
    loads = [pltpu.make_async_copy(a, b, loc.at[i]) for i, (a, b) in enumerate(loads)]
    for one in loads:
        one.start()
    gains[t] = jnp.broadcast_to(mg[...], (16, VD))
    for one in loads[:8]:
        one.wait()
    pl.semaphore_wait(barrier, 7)

    pending = []

    def copy(src, dst, ss, rs, dev):
        return pltpu.make_async_remote_copy(
            src_ref=src, dst_ref=dst, send_sem=ss, recv_sem=rs, device_id=dev, device_id_type=MESH
        )

    def send(src, dst, ss, rs, dev):
        one = copy(src, dst, ss, rs, dev)
        one.start()
        pending.append(one)

    def got(ref, ss, rs):
        copy(ref, ref, ss, rs, pc).wait_recv()

    def b_first(which, hop):
        dev, ss, rs, last, step = (
            (ym, b1m_s, b1m_r, YM, 1) if which else (yp, b1p_s, b1p_r, YP, -1)
        )
        shard = y if hop < 0 else ring(y, step * (hop + 1), 8)
        ref = bbuf.at[z, shard]
        if hop >= 0:
            got(ref, ss.at[hop], rs.at[hop])
        if hop + 1 < last:
            send(ref, ref, ss.at[hop + 1], rs.at[hop + 1], dev)
        if hop >= 0 or which:
            copy(ref, ref, b20_s, b20_r, zm).start()

    def a_first(which, hop):
        dev, ss, rs, last, step = (
            (zm, a1m_s, a1m_r, ZM, 1) if which else (zp, a1p_s, a1p_r, ZP, -1)
        )
        shard = z if hop < 0 else ring(z, step * (hop + 1), 8)
        ref = abuf.at[shard, y]
        if hop >= 0:
            got(ref, ss.at[hop], rs.at[hop])
        if hop + 1 < last:
            send(ref, ref, ss.at[hop + 1], rs.at[hop + 1], dev)
        if hop >= 0 or which:
            copy(ref, ref, a20_s, a20_r, ym).start()

    def b_part(row, k):
        return bbuf.at[row, :, :, 0:GU] if k == 0 else bbuf.at[row, :, :, GU:BW]

    def a_part(col, k):
        return abuf.at[:, col, :, 0:GU] if k == 0 else abuf.at[:, col, :, GU:AW]

    def b_second(which, hop, part):
        dev, ss, rs, last, step = (
            (zm, b2m_s, b2m_r, ZM, 1) if which else (zp, b2p_s, b2p_r, ZP, -1)
        )
        row = ring(z, step * (hop + 1), 8)
        if hop == 0 and which:
            got(bbuf.at[row], b20_s, b20_r)
        else:
            got(b_part(row, part), ss.at[hop, part], rs.at[hop, part])
        for k in (0, 1) if hop == 0 and which else (part,):
            if hop + 1 < last:
                ref = b_part(row, k)
                send(ref, ref, ss.at[hop + 1, k], rs.at[hop + 1, k], dev)

    def a_second(which, hop, part):
        dev, ss, rs, last, step = (
            (ym, a2m_s, a2m_r, YM, 1) if which else (yp, a2p_s, a2p_r, YP, -1)
        )
        col = ring(y, step * (hop + 1), 8)
        if hop == 0 and which:
            got(abuf.at[:, col], a20_s, a20_r)
        else:
            got(a_part(col, part), ss.at[hop, part], rs.at[hop, part])
        for k in (0, 1) if hop == 0 and which else (part,):
            if hop + 1 < last:
                ref = a_part(col, k)
                send(ref, ref, ss.at[hop + 1, k], rs.at[hop + 1, k], dev)

    def a_own():
        for k in (0, 1):
            ref = a_part(y, k)
            send(ref, ref, a2p_s.at[0, k], a2p_r.at[0, k], yp)

    def b_own():
        for k in (0, 1):
            ref = b_part(z, k)
            send(ref, ref, b2p_s.at[0, k], b2p_r.at[0, k], zp)

    def kinds(part):
        return ((0, kbuf), (2, gbuf)) if part == 0 else ((1, vbuf),)

    def kv_start(slot, part):
        to = slot + 1 + wrap
        return [
            copy(buf.at[slot], buf.at[to], kv_s.at[i, slot + 1], kv_r.at[i, to], turn)
            for i, buf in kinds(part)
        ]

    def kv_pass(slot, part):
        here = slot + REACH
        return [
            copy(buf.at[here], buf.at[slot], kv_s.at[i, here], kv_r.at[i, slot], yp)
            for i, buf in kinds(part)
        ]

    def kv_got(slot, part):
        for i, buf in kinds(part):
            got(buf.at[slot], kv_s.at[i, slot], kv_r.at[i, slot])

    def kv(slot, part, late):
        @pl.when(y < slot if late else y >= slot)
        def _():
            kv_got(slot, part)
            if slot < REACH:
                for one in kv_start(slot, part):
                    one.start()

    def kv_own(part):
        for one in kv_start(0, part):
            one.start()

    def relay(slot, part):
        @pl.when(last)
        def _():
            kv_got(slot + REACH, part)
            for one in kv_pass(slot, part):
                one.start()

    def kv_done():
        for slot in range(REACH):
            for part in (0, 1):
                for one in kv_start(slot, part):
                    one.wait_send()

        @pl.when(last)
        def _():
            for slot in range(REACH):
                for part in (0, 1):
                    for one in kv_pass(slot + 1, part):
                        one.wait_send()

    def attend(k, first, last):
        ids = gbuf[k].astype(F32) + jnp.where(s >= k, 0.0, 1000.0)

        def chunk(i, carry):
            rows = pl.ds(pl.multiple_of(i * QU, QU), QU)
            same = segq[rows, 0:1] == ids
            if k == 0:
                qpos = i * QU + lax.broadcasted_iota(jnp.int32, (QU, ROWS), 0)
                same = same & (lax.broadcasted_iota(jnp.int32, (QU, ROWS), 1) <= qpos)
            for m, q in enumerate((q1, q2)):
                score = dot_nt(q[rows, :], kbuf[k, :, m * HD : (m + 1) * HD])
                score = jnp.where(same, score * (HD**-0.5 * 1.4426950408889634), -jnp.inf)
                top = jnp.max(score, axis=1, keepdims=True)
                if k > 0:
                    before = mref[m, rows, 0:1]
                    top = jnp.maximum(top, before)
                expo = jnp.exp2(score - top)
                total = jnp.sum(expo, axis=1, keepdims=True)
                value = dot(expo.astype(BF), vbuf[k])
                if k > 0:
                    scale = jnp.exp2(before - top)
                    total = total + scale * lref[m, rows, 0:1]
                    value = value + scale * oacc[m, rows, :]
                mref[m, rows, :] = jnp.broadcast_to(top, (QU, 128))
                lref[m, rows, :] = jnp.broadcast_to(total, (QU, 128))
                oacc[m, rows, :] = value
            return carry

        lax.fori_loop(first, last, chunk, 0)

    def finish_heads(h):
        def chunk(i, carry):
            rows = pl.ds(pl.multiple_of(i * 64, 64), 64)
            head = oacc[0, rows, :] / lref[0, rows, 0:1]
            head = head - lam[0] * (oacc[1, rows, :] / lref[1, rows, 0:1])
            meansq = jnp.mean(head * head, axis=1, keepdims=True)
            heads[t, rows, :] = (head * lax.rsqrt(meansq + 1e-05) * hg[...]).astype(BF)
            return carry

        lax.fori_loop(h * 3, h * 3 + 3, chunk, 0)

    def slot_of(by, core):
        return ring(x, by, 4) * 2 + core

    def x_gather(buf, g, first, n):
        low, high = pl.ds(first, n // 2), pl.ds(first + n // 2, n // 2)
        both = pl.ds(first, n)

        def go(ref, i, dev):
            send(ref, ref, xg_s.at[g, i], xg_r.at[g, i], dev)

        def come(ref, i):
            got(ref, xg_s.at[g, i], xg_r.at[g, i])

        def own():
            mine = buf.at[t, both]
            go(mine, 0, xp)
            go(mine, 1, xm)
            go(mine, 4, pc)

        def near():
            a, b = buf.at[slot_of(-1, c), both], buf.at[slot_of(1, c), both]
            come(a, 0)
            go(buf.at[slot_of(-1, c), low], 2, xp)
            go(a, 5, pc)
            come(b, 1)
            go(buf.at[slot_of(1, c), high], 3, xm)
            go(b, 6, pc)

        def far():
            for i, part in ((2, low), (3, high)):
                ref = buf.at[slot_of(2, c), part]
                come(ref, i)
                go(ref, i + 5, pc)

        def across():
            come(buf.at[slot_of(0, o), both], 4)
            come(buf.at[slot_of(-1, o), both], 5)
            come(buf.at[slot_of(1, o), both], 6)

        def across_far():
            for i, part in ((2, low), (3, high)):
                come(buf.at[slot_of(2, o), part], i + 5)

        return own, near, far, across, across_far

    gain_g = x_gather(gains, 0, 0, 16)
    head_g = [x_gather(heads, 1 + h, h * CH, CH) for h in (0, 1)]
    mid_g = [x_gather(mids, 3 + h, h * CH, CH) for h in (0, 1)]

    def project(h, slots, first):
        rows = pl.ds(h * CH, CH)
        total = None if first else oacc[0, rows, :]
        for by, core in slots:
            i = slot_of(by, core)
            w = wout[pl.ds(pl.multiple_of(i * VD, VD), VD), :]
            part = dot(heads[i, rows, :], w)
            total = part if total is None else total + part
        return rows, total

    def project_near(h):
        slots = ((0, c), (-1, c), (1, c), (0, o), (-1, o), (1, o))
        rows, total = project(h, slots, True)
        oacc[0, rows, :] = total

    def project_far(h):
        rows, total = project(h, ((2, c), (2, o)), False)
        mids[t, rows, :] = (resid[rows, :].astype(F32) + total).astype(BF)

    def normalise(h):
        def chunk(i, carry):
            rows = pl.ds(pl.multiple_of(i * 32, 32), 32)
            mid = [mids[j, rows, :].astype(F32) for j in range(8)]
            squares = sum([m * m for m in mid])
            meansq = jnp.sum(squares, axis=1, keepdims=True) * (1.0 / (8 * VD))
            scale = lax.rsqrt(meansq + 1e-06)
            for j in range(8):
                gain = gains[j][0:1, :]
                xn[rows, j * VD : (j + 1) * VD] = (mid[j] * scale * gain).astype(BF)
            return carry

        lax.fori_loop(h * 6, h * 6 + 6, chunk, 0)

    def hidden(h):
        rows = pl.ds(h * CH, CH)

        def tile(i, carry):
            cols = pl.ds(pl.multiple_of(i * 256, 256), 256)
            gate = dot(xn[rows, :], bbuf[:, :, :, cols].reshape(2048, 256))
            up = dot(xn[rows, :], abuf[:, :, :, cols].reshape(2048, 256))
            hid[rows, cols] = (gate / (1.0 + jnp.exp(-gate)) * up).astype(BF)
            return carry

        lax.fori_loop(0, 3, tile, 0)

    def terms(i, core):
        i = slot_of((2, 1, -1, 0)[i], core)
        one = dot_nt(hid[:, 0 : BW - GU], bbuf[i, :, :, GU:BW].reshape(VD, BW - GU))
        two = dot_nt(hid[:, BW - GU :], abuf[i, :, :, GU:AW].reshape(VD, AW - GU))
        return one + two

    low, high = pl.ds(0, CH), pl.ds(CH, CH)

    def down(i):
        psend[i] = terms(i, o).astype(BF)
        send(psend.at[i], precv.at[i], d_s.at[i], d_r.at[i], pc)
        pown[i] = terms(i, c)

    def cross(i):
        got(precv.at[i], d_s.at[i], d_r.at[i])

    def chip_sum(i, part):
        return pown[i, part, :] + precv[i, part, :].astype(F32)

    def go(i, part, value, to, k, dev):
        stage[i, part, :] = value.astype(BF)
        send(stage.at[i, part], to.at[part], rs_s.at[k], rs_r.at[k], dev)

    def come(ref, part, k):
        got(ref.at[part], rs_s.at[k], rs_r.at[k])

    def sum_0():
        cross(0)
        go(0, low, chip_sum(0, low), rhalf, 0, xp)
        go(0, high, chip_sum(0, high), rhalf, 1, xm)

    def sum_1():
        cross(1)
        go(1, high, chip_sum(1, high), rfull.at[0], 2, xp)

    def sum_2():
        cross(2)
        go(2, low, chip_sum(2, low), rfull.at[1], 3, xm)

    def sum_3():
        come(rhalf, low, 0)
        go(1, low, chip_sum(1, low) + rhalf[low, :].astype(F32), rfull.at[0], 4, xp)
        come(rhalf, high, 1)
        go(2, high, chip_sum(2, high) + rhalf[high, :].astype(F32), rfull.at[1], 5, xm)

    def sum_4():
        cross(3)
        pown[3] = pown[3] + precv[3].astype(F32) + mids[t].astype(F32)
        for part, i, k in ((high, 0, 2), (low, 1, 3)):
            come(rfull.at[i], part, k)
            pown[3, part, :] += rfull[i, part, :].astype(F32)
        for part, i, k in ((low, 0, 4), (high, 1, 5)):
            come(rfull.at[i], part, k)
            out_ref[part, :] = (pown[3, part, :] + rfull[i, part, :].astype(F32)).astype(BF)

    events = []

    def at(time, what, *args):
        events.append((time, len(events), what, args))

    for which, first in ((True, b_first), (True, a_first)):
        for hop, time in enumerate((3.4, 6.7, 11.4, 16.2, 19.5)):
            at(time, first, True, hop)
    for first in (b_first, a_first):
        at(3.5, first, False, 0)
        at(9.2 if first is b_first else 6.8, first, False, 1)
    at(2.0, gain_g[0])
    at(7.5, gain_g[1])
    at(11.0, gain_g[2])
    at(11.5, gain_g[3])
    at(14.5, gain_g[4])
    at(2.1, attend, 0, 0, 4)
    at(3.6, kv_own, 1)
    for slot, (tk, tv) in enumerate(((9.0, 14.0), (18.4, 22.6), (26.8, 31.0), (35.2, 39.4))):
        for part, time in enumerate((tk, tv)):
            at(time, relay, slot + 1, part)
            at(time, kv, slot + 1, part, False)
        at(tk + 6.5, kv, slot + 1, 0, True)
        at(tv + 6.5, kv, slot + 1, 1, True)
        if slot < 3:
            at(tv + 6.6, attend, slot + 1, 0, 4)
    at(39.5, a_own)
    at(31.2, b_own)
    for second in (a_second, b_second):
        times = ((23.0, 23.0), (32.75, 37.0), (45.0, 49.5), (57.5, 61.0), (73.0, 77.5))
        for hop, pair in enumerate(times):
            for part in (0,) if hop == 0 else (0, 1):
                at(pair[part], second, True, hop, part)
    for hop, pair in enumerate(((53.0, 57.0), (66.0, 70.0))):
        for part in (0, 1):
            at(pair[part], a_second, False, hop, part)
    for hop, pair in enumerate(((45.5, 50.0), (60.0, 64.0))):
        for part in (0, 1):
            at(pair[part], b_second, False, hop, part)
    for h, late in ((0, 7.5), (1, 9.5)):
        at(38.7 + late, attend, REACH, 2 * h, 2 * h + 2)
        at(38.8 + late, finish_heads, h)
        at(38.9 + late, head_g[h][0])
        at(43.0 + late, head_g[h][1])
        at(44.8 + late, head_g[h][3])
        at(44.9 + late, project_near, h)
        at(46.0 + late, head_g[h][2])
        at(47.4 + late, head_g[h][4])
        at(47.5 + late, project_far, h)
        at(47.6 + late, mid_g[h][0])
        at(51.8 + late, mid_g[h][1])
        at(54.8 + late, mid_g[h][2])
        at(56.0 + late, mid_g[h][3])
        at(56.1 + late, mid_g[h][4])
        at(56.2 + late, normalise, h)

    def drain():
        while pending:
            pending.pop(0).wait_send()
        kv_done()
        copy(bbuf.at[z], bbuf.at[z], b20_s, b20_r, zm).wait_send()
        copy(abuf.at[:, y], abuf.at[:, y], a20_s, a20_r, ym).wait_send()

    at(72.9, drain)
    at(74.0, hidden, 0)
    at(74.1, hidden, 1)
    tail = (
        (down, 0), (down, 1), (sum_0,), (down, 2), (sum_1,), (down, 3), (sum_2,), (sum_3,), (sum_4,)
    )
    for i, one in enumerate(tail):
        at(78.0 + i, *one)

    b_first(True, -1)
    b_first(False, -1)
    a_first(True, -1)
    a_first(False, -1)
    kv_own(0)
    for one in loads[8:]:
        one.wait()
    ids = jnp.broadcast_to(gbuf[0].astype(F32), (128, ROWS))
    segq[...] = ids.T
    for _, _, what, args in sorted(events, key=lambda e: e[:2]):
        what(*args)

    for one in pending:
        one.wait_send()


def body(
    resid, query_one, key_one, query_two, key_two, values, mix_lambda, segments, head_gain,
    out_weight, mixer_gain, gate_weight, up_weight, down_weight,
):
    hbm = pl.BlockSpec(memory_space=pltpu.HBM)
    vmem = pl.BlockSpec(memory_space=pltpu.VMEM)
    dma = pltpu.SemaphoreType.DMA
    scratch = [
        pltpu.VMEM((ROWS, HD), BF), pltpu.VMEM((ROWS, HD), BF), pltpu.VMEM((ROWS, VD), BF),
        pltpu.VMEM((2048, VD), BF),
        pltpu.VMEM((9, ROWS, 2 * HD), BF), pltpu.VMEM((9, ROWS, VD), BF),
        pltpu.VMEM((9, 1, ROWS), jnp.int32),
        pltpu.VMEM((8, 8, 32, BW), BF), pltpu.VMEM((8, 8, 32, AW), BF),
        pltpu.VMEM((ROWS, 128), F32), pltpu.VMEM((8, 16, VD), F32),
        pltpu.VMEM((2, ROWS, 128), F32), pltpu.VMEM((2, ROWS, 128), F32),
        pltpu.VMEM((2, ROWS, VD), F32),
        pltpu.VMEM((8, ROWS, VD), BF), pltpu.VMEM((8, ROWS, VD), BF),
        pltpu.VMEM((ROWS, 2048), BF), pltpu.VMEM((ROWS, 768), BF),
        pltpu.VMEM((4, ROWS, VD), F32), pltpu.VMEM((4, ROWS, VD), BF),
        pltpu.VMEM((4, ROWS, VD), BF), pltpu.VMEM((3, ROWS, VD), BF),
        pltpu.VMEM((ROWS, VD), BF), pltpu.VMEM((2, ROWS, VD), BF),
        dma((12,)), dma((3, 9)), dma((3, 9)),
        dma((YM,)), dma((YM,)), dma((YP,)), dma((YP,)),
        dma((ZM,)), dma((ZM,)), dma((ZP,)), dma((ZP,)),
        dma, dma, dma, dma,
        dma((ZM, 2)), dma((ZM, 2)), dma((ZP, 2)), dma((ZP, 2)),
        dma((YM, 2)), dma((YM, 2)), dma((YP, 2)), dma((YP, 2)),
        dma((5, 9)), dma((5, 9)), dma((4,)), dma((4,)), dma((6,)), dma((6,)),
    ]
    return pl.pallas_call(
        kernel,
        name="layer",
        out_shape=jax.ShapeDtypeStruct((ROWS, VD), BF),
        in_specs=[hbm] * 11 + [vmem] * 2 + [pl.BlockSpec(memory_space=pltpu.SMEM)],
        out_specs=vmem,
        scratch_shapes=scratch,
        compiler_params=pltpu.CompilerParams(collective_id=0, has_side_effects=True),
    )(
        query_one, query_two, key_one, key_two, values, resid, out_weight, gate_weight,
        up_weight, down_weight.T, segments, head_gain.reshape(1, -1),
        mixer_gain.reshape(1, -1), mix_lambda,
    )


def solution(mesh):
    in_specs = (
        P("sp", "tp"), P("sp", "tp"), P("sp", "tp"), P("sp", "tp"), P("sp", "tp"), P("sp", "tp"),
        P("tp"), P("sp"), P(), P(None, "tp"), P("tp"), P("sp", "tp"), P("sp", "tp"), P("tp", "sp"),
    )
    return jax.shard_map(
        body, mesh=mesh, in_specs=in_specs, out_specs=P("sp", "tp"), check_vma=False
    )
```
